32 devices in a mesh: sp: 8 (over z, core), tp: 4 (over y, x).
Axes of the slice: x: 2, y: 2, z: 4, core: 2. Of those that a mesh axis runs over, the one named last changes fastest.
Arguments:
- moe_input: bfloat16 [1408, 2048], P('sp'), may hold values from -6 to 6
- cotangent: bfloat16 [1408, 2048], P('sp'), may hold values from -6 to 6
- route_ids: int32 [1408, 2], P('sp'), may hold values from 0 to 7, all different within a row; in each aligned block of 176 rows (0 to 175, 176 to 351, ...) at most 88 rows name the same one
- route_weights: float32 [1408, 2], P('sp'), may hold values from 0.25 to 1.5
- expert_gate: bfloat16 [8, 2048, 1024], P('sp', None, 'tp'), may hold values from -0.125 to 0.125
- expert_up: bfloat16 [8, 2048, 1024], P('sp', None, 'tp'), may hold values from -0.125 to 0.125
- expert_down: bfloat16 [8, 1024, 2048], P('sp', 'tp'), may hold values from -0.1875 to 0.1875
- out_proj: bfloat16 [2048, 2048], P('tp'), may hold values from -0.125 to 0.125
- gate_b: bfloat16 [1408, 2048], P('sp', 'tp'), may hold values from -6 to 6
- gate_c: bfloat16 [1408, 2048], P('sp', 'tp'), may hold values from -6 to 6
- conv_in: bfloat16 [1408, 2048], P('sp', 'tp'), may hold values from -6 to 6
- taps: float32 [3, 2048], P(None, 'tp'), may hold values from -4 to 4
Outputs:
- grad_expert_gate: float32 [8, 2048, 1024], P('sp', None, 'tp')
- grad_expert_up: float32 [8, 2048, 1024], P('sp', None, 'tp')
- grad_expert_down: float32 [8, 1024, 2048], P('sp', 'tp')
- grad_out_proj: float32 [2048, 2048], P('tp', 'sp')
- grad_gate_b: bfloat16 [1408, 2048], P('sp', 'tp')
- grad_gate_c: bfloat16 [1408, 2048], P('sp', 'tp')
- grad_conv_in: bfloat16 [1408, 2048], P('sp', 'tp')
The draws below stay inside these ranges and needn't reach their ends.
Inputs may be any that keep to these rules, and one draw needn't show every extreme that they name: `route_ids`: in the 176 rows of each index of sp, each row names 2 different experts, no expert is named by more than 88 rows, a bound that some block reaches.
All inputs are finite; a program needn't handle non-finite values.
Results may differ from the reference program's by a relative error of at most 0.033.
Values may be sent and summed in bfloat16 or wider, within the bound.
A program may use at most 64 MiB of HBM per device.

```python
import math
import jax
import jax.numpy as jnp
import numpy as np
from jax import lax

D = 2048
FF = 1024
TOPK = 2
TAPS = 3
TOK_SP = 176
TOKENS = 1408
EXPERTS = 8
CAP = 88
N_SP = 8
N_TP = 4


def raised(array, own_key, source, target, parts, factor):
    owner, partner = [(jnp.arange(array.shape[axis_at]) // (array.shape[axis_at] // parts)).reshape([-1 if axis == axis_at else 1 for axis in range(array.ndim)]) for axis_at in (source, target)]
    chosen = jax.random.permutation(own_key, parts)[partner]
    strong = (owner == chosen) | (owner == (partner + parts // 2) % parts)
    return jnp.where(strong, factor * array, array)


def block_scale(key, extent, cuts, low, top_value):
    def one(dim, parts):
        heights = jax.random.uniform(jax.random.fold_in(jax.random.fold_in(key, 6), dim), (parts,), jnp.float32, low / len(cuts), top_value / len(cuts))
        return jnp.repeat(jnp.exp(heights), extent[dim] // parts).reshape((-1,) + (1,) * (len(extent) - dim - 1))

    gain = one(*cuts[0])
    for cut in cuts[1:]:
        gain = gain * one(*cut)
    return gain


def shared_out(own_key, own, number, rows, count, top, reach, skew):
    sequence = jax.random.permutation(own_key, count)
    crowded, common = shares(count, rows * top, reach, skew, True), shares(count, rows * top, reach, skew, False)
    places = jnp.arange(count)

    def named(lengths, rotation):
        used = int((lengths > 0).sum())
        fixed = max(1, used // 4)
        passed = fixed + (places - fixed + rotation * (used - fixed)) % max(1, count - fixed)
        return jnp.zeros((count,), jnp.int32).at[sequence[jnp.where(places < fixed, places, passed)]].set(jnp.asarray(lengths, jnp.int32))

    lengths = jnp.where(number % 4 == 0, named(crowded, number // 4), named(common, number - number // 4 - 1))
    mixed = jax.random.permutation(jax.random.fold_in(own, 3), count)
    source_of, receiver = mixed[0:count // 2 * 2:2], mixed[1:count // 2 * 2:2]
    room = jnp.minimum(lengths[source_of] - 1, reach - lengths[receiver]) // 2
    room = jnp.where((source_of == sequence[0]) | (receiver == sequence[0]) | (lengths[receiver] == 0), 0, jnp.maximum(room, 0))
    passed = jax.random.randint(jax.random.fold_in(own, 4), (count // 2,), 0, 1 << 20) % (room + 1)
    lengths = lengths.at[source_of].add(-passed).at[receiver].add(passed)
    items = jnp.searchsorted(jnp.cumsum(lengths), jnp.arange(rows * top), side="right").astype(jnp.int32)
    grid = items.reshape(top, rows).T
    grid = grid[jax.random.permutation(jax.random.fold_in(own, 1), rows)]
    rotation = jax.random.randint(jax.random.fold_in(own, 2), (rows, 1), 0, top)
    return jnp.take_along_axis(grid, (jnp.arange(top)[None, :] + rotation) % top, axis=1)


def shares(amount, total, limit, slope, full):
    portions = [(1 << 20) // math.isqrt(standing ** slope) + 1 for standing in range(1, amount + 1)]
    largest = limit if full else min(limit, max(-(-total // amount), total * portions[0] // sum(portions)))
    least = 1 if total - largest >= amount - 1 else 0
    counts, rest = [largest] + [least] * (amount - 1), total - largest - least * (amount - 1)
    while rest > 0:
        candidates = [i for i in range(1, amount) if counts[i] < largest] or [i for i in range(1, amount) if counts[i] < limit]
        pool, left = sum([portions[i] for i in candidates]), rest
        for i in candidates:
            extra = min(limit - counts[i], max(1, left * portions[i] // pool), rest)
            counts[i] = counts[i] + extra
            rest = rest - extra
    return np.array(counts)


def scatter_about(own_key, extent, deviation, bound, shards=(), kind=jnp.bfloat16):
    entries = deviation * jax.random.normal(own_key, extent, jnp.float32)
    if shards:
        entries = entries * block_scale(own_key, extent, shards, -0.22, 0.18)
    return jnp.clip(entries, -bound, bound).astype(kind)


def bell_draw_with(rng, extent, spread, bound, split, heavy, held_as=jnp.bfloat16):
    entries = spread * jax.random.normal(rng, extent, jnp.float32)
    if split:
        entries = entries * block_scale(rng, extent, split, -0.22, 0.18)
    return jnp.clip(raised(entries, jax.random.fold_in(rng, 3), *heavy), -bound, bound).astype(held_as)


def setup_inputs(seed: int = 0) -> dict:
    streams_of = jax.random.split(jax.random.key(seed), 13)
    moe_input = scatter_about(streams_of[0], (TOKENS, D), 1.0, 6.0, ((0, 8),))
    cotangent = bell_draw_with(streams_of[1], (TOKENS, D), 1.0, 6.0, ((0, 8),), (0, 1, 8, 2.0))
    route_ids_keys = jax.random.split(jax.random.fold_in(streams_of[2], 1), TOKENS // TOK_SP)
    route_ids_turns = jax.random.permutation(jax.random.fold_in(streams_of[2], 3), TOKENS // TOK_SP)
    route_ids = jax.vmap(lambda own, number: shared_out(jax.random.fold_in(streams_of[2], 2), own, number, TOK_SP, EXPERTS, TOPK, CAP, 2))(route_ids_keys, route_ids_turns).reshape((TOKENS, TOPK))
    route_weights = jnp.clip(0.25 + 1.25 * jax.random.uniform(streams_of[3], (TOKENS, TOPK), jnp.float32) ** block_scale(streams_of[3], (TOKENS, TOPK), ((0, 8),), -0.2, 0.2), 0.25, 1.5)
    expert_gate = scatter_about(streams_of[4], (EXPERTS, D, FF), D ** -0.5, 0.125, ((0, 8), (2, 4)))
    expert_up = scatter_about(streams_of[5], (EXPERTS, D, FF), D ** -0.5, 0.125, ((0, 8), (2, 4)))
    expert_down = scatter_about(streams_of[6], (EXPERTS, FF, D), FF ** -0.5, 0.1875, ((0, 8), (1, 4)))
    out_proj = scatter_about(streams_of[7], (D, D), D ** -0.5, 0.125, ((0, 4),))
    gate_b = scatter_about(streams_of[8], (TOKENS, D), 1.0, 6.0, ((0, 8), (1, 4)))
    gate_c = scatter_about(streams_of[9], (TOKENS, D), 1.0, 6.0, ((0, 8), (1, 4)))
    conv_in = scatter_about(streams_of[10], (TOKENS, D), 1.0, 6.0, ((0, 8), (1, 4)))
    taps = scatter_about(streams_of[11], (TAPS, D), 0.6, 4.0, ((1, 4),), jnp.float32)
    return {"moe_input": moe_input, "cotangent": cotangent, "route_ids": route_ids, "route_weights": route_weights, "expert_gate": expert_gate, "expert_up": expert_up, "expert_down": expert_down, "out_proj": out_proj, "gate_b": gate_b, "gate_c": gate_c, "conv_in": conv_in, "taps": taps}


def slot_table(routes, experts, capacity):
    flattened = routes.reshape(-1)
    onehot = (flattened[:, None] == jnp.arange(experts, dtype=jnp.int32)[None, :]).astype(jnp.int32)
    earlier = jnp.cumsum(onehot, axis=0) - onehot
    return flattened * capacity + jnp.sum(earlier * onehot, axis=1)


def expert_backward(packed):
    rows_x, rows_s, weight_gate, weight_up, weight_down = packed
    pre_gate = jnp.dot(rows_x, weight_gate, preferred_element_type=jnp.float32)
    pre_up = jnp.dot(rows_x, weight_up, preferred_element_type=jnp.float32)
    sigma = jax.nn.sigmoid(pre_gate)
    active = pre_gate * sigma
    hidden = (active * pre_up).astype(jnp.bfloat16)
    back = jnp.dot(rows_s, weight_down.T, preferred_element_type=jnp.float32)
    grad_pre_gate = (back * pre_up * sigma * (1.0 + pre_gate * (1.0 - sigma))).astype(jnp.bfloat16)
    grad_pre_up = (back * active).astype(jnp.bfloat16)
    grad_down = jnp.dot(hidden.T, rows_s, preferred_element_type=jnp.float32)
    grad_gate = jnp.dot(rows_x.T, grad_pre_gate, preferred_element_type=jnp.float32)
    grad_up = jnp.dot(rows_x.T, grad_pre_up, preferred_element_type=jnp.float32)
    piece = FF // N_TP
    split_gate = grad_pre_gate.astype(jnp.float32).reshape(-1, N_TP, piece)
    split_up = grad_pre_up.astype(jnp.float32).reshape(-1, N_TP, piece)
    wide_gate = weight_gate.astype(jnp.float32).reshape(D, N_TP, piece)
    wide_up = weight_up.astype(jnp.float32).reshape(D, N_TP, piece)
    partial_value = jnp.einsum('sti,dti->tsd', split_gate, wide_gate) + jnp.einsum('sti,dti->tsd', split_up, wide_up)
    slot_grad = jnp.sum(partial_value.astype(jnp.bfloat16).astype(jnp.float32), axis=0).astype(jnp.bfloat16)
    return grad_gate, grad_up, grad_down, slot_grad


def reference(moe_input, cotangent, route_ids, route_weights, expert_gate, expert_up, expert_down, out_proj, gate_b, gate_c, conv_in, taps):
    assigned = TOKENS * TOPK
    blocks = route_ids.reshape(N_SP, TOK_SP * TOPK)
    local = jax.vmap(lambda ids: slot_table(ids, EXPERTS, CAP))(blocks)
    source = jnp.arange(N_SP, dtype=jnp.int32)[:, None]
    global_slot = (blocks * (N_SP * CAP) + source * CAP + (local - blocks * CAP)).reshape(-1).astype(jnp.int32)
    owner = jnp.full((EXPERTS * N_SP * CAP,), assigned, jnp.int32).at[global_slot].set(jnp.arange(assigned, dtype=jnp.int32))
    token_owner = jnp.where(owner < assigned, owner // TOPK, TOKENS).astype(jnp.int32)
    scaled = (route_weights[:, :, None] * cotangent[:, None, :].astype(jnp.float32)).astype(jnp.bfloat16).reshape(assigned, D)
    padded_x = jnp.concatenate([moe_input, jnp.zeros((1, D), jnp.bfloat16)], axis=0)
    padded_s = jnp.concatenate([scaled, jnp.zeros((1, D), jnp.bfloat16)], axis=0)
    slots_x = padded_x[token_owner].reshape(EXPERTS, N_SP * CAP, D)
    slots_s = padded_s[owner].reshape(EXPERTS, N_SP * CAP, D)
    grad_gate, grad_up, grad_down, slot_grad = lax.map(expert_backward, (slots_x, slots_s, expert_gate, expert_up, expert_down))
    slot_rows = slot_grad.reshape(-1, D)
    moe_rows = slot_rows[global_slot].astype(jnp.float32).reshape(TOKENS, TOPK, D).sum(axis=1)
    stream_grad = (cotangent.astype(jnp.float32) + moe_rows).astype(jnp.bfloat16)
    mixed = gate_c.astype(jnp.float32) * conv_in.astype(jnp.float32)
    mixed_pad = jnp.pad(mixed, ((2, 0), (0, 0)))
    conv = taps[2] * mixed + taps[1] * mixed_pad[1:-1] + taps[0] * mixed_pad[:-2]
    merged = (gate_b.astype(jnp.float32) * conv).astype(jnp.bfloat16)
    grad_merged = jnp.dot(stream_grad, out_proj.T, preferred_element_type=jnp.float32)
    grad_gate_b = (grad_merged * conv).astype(jnp.bfloat16)
    grad_conv = grad_merged * gate_b.astype(jnp.float32)
    grad_pad = jnp.pad(grad_conv, ((0, 2), (0, 0)))
    grad_mixed = taps[2] * grad_conv + taps[1] * grad_pad[1:-1] + taps[0] * grad_pad[2:]
    grad_gate_c = (grad_mixed * conv_in.astype(jnp.float32)).astype(jnp.bfloat16)
    grad_conv_in = (grad_mixed * gate_c.astype(jnp.float32)).astype(jnp.bfloat16)
    grad_out_proj = jnp.dot(merged.T, stream_grad, preferred_element_type=jnp.float32)
    return (grad_gate, grad_up, grad_down, grad_out_proj, grad_gate_b, grad_gate_c, grad_conv_in)
```

```python
import functools
import jax
import jax.numpy as jnp
from jax import lax
from jax.experimental import pallas as pl
from jax.experimental.pallas import tpu as pltpu
from jax.sharding import PartitionSpec as P

EXP_DEV = 1


def passed_along(block, axis, distance):
    devices = range(lax.axis_size(axis))
    route = [(i - distance, i) for i in devices if i - distance in devices]
    return lax.ppermute(block, axis, route)


def slot_table(routes, experts, capacity):
    flattened = routes.reshape(-1)
    onehot = (flattened[:, None] == jnp.arange(experts, dtype=jnp.int32)[None, :]).astype(jnp.int32)
    earlier = jnp.cumsum(onehot, axis=0) - onehot
    return flattened * capacity + jnp.sum(earlier * onehot, axis=1)


def contract(left, right, left_dim, right_dim):
    return lax.dot_general(
        left, right, (((left_dim,), (right_dim,)), ((), ())), preferred_element_type=jnp.float32
    )


def slot_plan(
    moe_input,
    cotangent,
    route_ids,
    route_weights,
    expert_gate,
    expert_up,
    expert_down,
    out_proj,
    gate_b,
    gate_c,
    conv_in,
    taps,
):
    groups = lax.axis_size("sp")
    lanes = lax.axis_size("tp")
    token_count, model_width = moe_input.shape
    choices_count = route_ids.shape[1]
    experts = EXP_DEV * groups
    capacity = 2 * token_count * choices_count // experts
    assigned = token_count * choices_count
    slice_width = model_width // lanes
    column_start = lax.axis_index("tp") * slice_width
    slots = slot_table(route_ids, experts, capacity)
    owner = (
        jnp.full((experts * capacity,), assigned, jnp.int32)
        .at[slots]
        .set(jnp.arange(assigned, dtype=jnp.int32))
    )
    token_owner = jnp.where(owner < assigned, owner // choices_count, token_count)
    scaled = (
        (route_weights[:, :, None] * cotangent[:, None, :].astype(jnp.float32))
        .astype(jnp.bfloat16)
        .reshape(assigned, model_width)
    )

    def to_slots(values, positions):
        padded = jnp.concatenate([values, jnp.zeros((1, values.shape[1]), values.dtype)], axis=0)
        return padded[positions].reshape(experts, capacity, values.shape[1])

    slim_x = to_slots(
        lax.dynamic_slice_in_dim(moe_input, column_start, slice_width, 1), token_owner
    )
    slim_s = to_slots(lax.dynamic_slice_in_dim(scaled, column_start, slice_width, 1), owner)
    part_x, part_s = (
        lax.all_to_all(slim_x, "sp", split_axis=0, concat_axis=0, tiled=True),
        lax.all_to_all(slim_s, "sp", split_axis=0, concat_axis=0, tiled=True),
    )
    arrived_x, arrived_s = (
        lax.all_gather(part_x, "tp", axis=2, tiled=True),
        lax.all_gather(part_s, "tp", axis=2, tiled=True),
    )
    rows_x = arrived_x.reshape(-1, model_width)
    rows_s = arrived_s.reshape(-1, model_width)
    weight_gate = expert_gate[0]
    weight_up = expert_up[0]
    weight_down = expert_down[0]
    pre_gate = jnp.dot(rows_x, weight_gate, preferred_element_type=jnp.float32)
    pre_up = jnp.dot(rows_x, weight_up, preferred_element_type=jnp.float32)
    sigma = jax.nn.sigmoid(pre_gate)
    active = pre_gate * sigma
    hidden = (active * pre_up).astype(jnp.bfloat16)
    back = contract(rows_s, weight_down, 1, 1)
    grad_pre_gate = (back * pre_up * sigma * (1.0 + pre_gate * (1.0 - sigma))).astype(jnp.bfloat16)
    grad_pre_up = (back * active).astype(jnp.bfloat16)
    grad_down = contract(hidden, rows_s, 0, 0)
    grad_gate = contract(rows_x, grad_pre_gate, 0, 0)
    grad_up = contract(rows_x, grad_pre_up, 0, 0)
    partial_value = contract(grad_pre_gate, weight_gate, 1, 1) + contract(
        grad_pre_up, weight_up, 1, 1
    )
    summed = lax.psum_scatter(
        partial_value.astype(jnp.bfloat16), "tp", scatter_dimension=1, tiled=True
    )
    returned = lax.all_to_all(
        summed.reshape(groups, capacity, slice_width), "sp", split_axis=0, concat_axis=0, tiled=True
    )
    returned = returned.reshape(experts * capacity, slice_width)
    moe_rows = (
        returned[slots]
        .astype(jnp.float32)
        .reshape(token_count, choices_count, slice_width)
        .sum(axis=1)
    )
    own_cols = lax.dynamic_slice_in_dim(cotangent, column_start, slice_width, 1)
    grad_cols = (own_cols.astype(jnp.float32) + moe_rows).astype(jnp.bfloat16)
    stream_grad = lax.all_gather(grad_cols, "tp", axis=1, tiled=True)
    mixed = gate_c.astype(jnp.float32) * conv_in.astype(jnp.float32)
    earlier_rows = passed_along(mixed[-2:], "sp", 1)
    extended = jnp.concatenate([earlier_rows, mixed], axis=0)
    conv = taps[2] * mixed + taps[1] * extended[1:-1] + taps[0] * extended[:-2]
    merged = (gate_b.astype(jnp.float32) * conv).astype(jnp.bfloat16)
    grad_merged = contract(stream_grad, out_proj, 1, 1)
    grad_gate_b = (grad_merged * conv).astype(jnp.bfloat16)
    grad_conv = grad_merged * gate_b.astype(jnp.float32)
    later_rows = passed_along(grad_conv[:2], "sp", -1)
    extended_grad = jnp.concatenate([grad_conv, later_rows], axis=0)
    grad_mixed = taps[2] * grad_conv + taps[1] * extended_grad[1:-1] + taps[0] * extended_grad[2:]
    grad_gate_c = (grad_mixed * conv_in.astype(jnp.float32)).astype(jnp.bfloat16)
    grad_conv_in = (grad_mixed * gate_c.astype(jnp.float32)).astype(jnp.bfloat16)
    grad_proj = lax.psum_scatter(
        contract(stream_grad, merged, 0, 0).astype(jnp.bfloat16),
        "sp",
        scatter_dimension=0,
        tiled=True,
    ).astype(jnp.float32)
    return (
        grad_gate[None],
        grad_up[None],
        grad_down[None],
        grad_proj.T,
        grad_gate_b,
        grad_gate_c,
        grad_conv_in,
    )


MESH = pl.DeviceIdType.MESH


def place():
    sp, t = lax.axis_index("sp"), lax.axis_index("tp")
    return sp, lax.div(sp, 2), lax.rem(sp, 2), t


def flipped(t, bits):
    x, y = lax.rem(t, 2), lax.div(t, 2)
    if bits & 1:
        x = 1 - x
    if bits & 2:
        y = 1 - y
    return 2 * y + x


def greet(devices):
    barrier = pltpu.get_barrier_semaphore()
    for device, exists in devices:
        @pl.when(exists)
        def _():
            pl.semaphore_signal(barrier, inc=1, device_id=device, device_id_type=MESH)
    pl.semaphore_wait(barrier, sum([jnp.where(exists, 1, 0) for _, exists in devices]))


def gather_kernel(
    stacks, x_ref, s_ref, m_ref, full_x, full_s, full_m,
    zs, zr, xs, xr, ys, yr, ax, ar, bx, br, cs, cr, own_s, own_r, local,
):
    sp, z, c, t = place()
    rows, width = x_ref.shape
    quarter = width // 4
    half = quarter // 2
    partner = (2 * z + 1 - c, t)
    up, down = (sp + 2, t), (sp - 2, t)
    tx, ty, td = flipped(t, 1), flipped(t, 2), flipped(t, 3)
    always = z >= 0
    greet([
        (partner, always), ((sp, tx), always), ((sp, ty), always),
        (up, z < stacks - 1), (down, z > 0),
    ])
    ins, outs = (x_ref, s_ref, m_ref), (full_x, full_s, full_m)

    def cols(q, part=None):
        if part is None:
            return pl.ds(pl.multiple_of(q * quarter, 128), quarter)
        return pl.ds(pl.multiple_of(q * quarter + part * half, 128), half)

    def span(d):
        return pl.ds(pl.multiple_of((2 * d + c) * rows, 16), rows)

    def remote(src, dst, send, recv, device):
        return pltpu.make_async_remote_copy(
            src_ref=src, dst_ref=dst, send_sem=send, recv_sem=recv,
            device_id=device, device_id_type=MESH,
        )

    def region(a, d, q, part=None):
        if a == 2:
            return outs[2].at[span(d), :]
        return outs[a].at[span(d), cols(q, part)]

    def mine(a):
        return m_ref if a == 2 else ins[a].at[:, cols(t)]

    def slot(a, way, k):
        return (a * 2 + way) * (stacks - 1) + k

    def zcopy(a, way, k, src, d):
        i = slot(a, way, k)
        return remote(src, region(a, d, t), zs.at[i], zr.at[i], up if way == 0 else down)

    def ahead(way):
        return z < stacks - 1 if way == 0 else z > 0

    def source(way, k):
        return z - 1 - k if way == 0 else z + 1 + k

    def exists(way, k):
        return z >= k + 1 if way == 0 else z + 1 + k < stacks

    order = (0, 1, 2)
    for a in order:
        for way in (0, 1):
            @pl.when(ahead(way))
            def _():
                zcopy(a, way, 0, mine(a), z).start()
    keeps = []
    for a in order:
        dst = outs[a].at[span(z), :]
        keeps.append(pltpu.make_async_copy(ins[a], dst, local.at[a]))
        keeps[-1].start()
        keeps.append(remote(ins[a], dst, own_s.at[a], own_r.at[a], partner))
        keeps[-1].start()

    def xy(a, way, k, d, kind):
        i = slot(a, way, k)
        if kind == "x":
            r = region(a, d, t)
            return remote(r, r, xs.at[i], xr.at[i], (sp, tx))
        if kind == "y":
            r = region(a, d, t)
            return remote(r, r, ys.at[i], yr.at[i], (sp, ty))
        if kind == "a":
            r = region(a, d, tx, 0)
            return remote(r, r, ax.at[i], ar.at[i], (sp, ty))
        r = region(a, d, ty, 1)
        return remote(r, r, bx.at[i], br.at[i], (sp, tx))

    def shared(a, way, k, d, which):
        i = 4 * slot(a, way, k) + which
        r = region(a, d, (t, tx, ty, td)[which])
        return remote(r, r, cs.at[i], cr.at[i], partner)

    def first(a, way, k):
        d = source(way, k)
        zcopy(a, way, k, region(a, d, t), d).wait_recv()
        if k < stacks - 2:
            @pl.when(ahead(way))
            def _():
                zcopy(a, way, k + 1, region(a, d, t), d).start()
        if a < 2:
            xy(a, way, k, d, "x").start()
            xy(a, way, k, d, "y").start()
        shared(a, way, k, d, 0).start()

    def second(a, way, k):
        d = source(way, k)
        if a < 2:
            xy(a, way, k, d, "x").wait_recv()
            xy(a, way, k, d, "a").start()
            shared(a, way, k, d, 1).start()
            xy(a, way, k, d, "y").wait_recv()
            xy(a, way, k, d, "b").start()
            shared(a, way, k, d, 2).start()

    def third(a, way, k):
        d = source(way, k)
        if a < 2:
            xy(a, way, k, d, "a").wait_recv()
            xy(a, way, k, d, "b").wait_recv()
            shared(a, way, k, d, 3).start()

    steps = [(a, way, k) for k in range(stacks - 1) for a in order for way in (0, 1)]
    for i in range(len(steps) + 4):
        for stage, lag in ((first, 0), (second, 2), (third, 4)):
            if 0 <= i - lag < len(steps):
                a, way, k = steps[i - lag]
                @pl.when(exists(way, k))
                def _():
                    stage(a, way, k)
    for copy in keeps:
        copy.wait()
    for a, way, k in steps:
        passed = z >= k if way == 0 else z + k < stacks

        @pl.when(passed & ahead(way))
        def _():
            d = z - k if way == 0 else z + k
            zcopy(a, way, k, region(a, d, t), d).wait_send()

        @pl.when(exists(way, k))
        def _():
            d = source(way, k)
            if a < 2:
                for kind in "xyab":
                    xy(a, way, k, d, kind).wait_send()
            for which in range(4 if a < 2 else 1):
                shared(a, way, k, d, which).wait()


def return_kernel(
    stacks, p_ref, c_ref, stream, columns,
    theirs, ours, summed, in_x, in_y, out_a, out_b, got_x, got_y, block, blocks, cols,
    ps, pr, as_, ar, bs, br, xs, xr, ys, yr, zs, zr, gs, gr, es, er, local, load,
):
    sp, z, c, t = place()
    rows, width = p_ref.shape[0] // (2 * stacks), p_ref.shape[1]
    quarter = width // 4
    half = quarter // 2
    partner = (2 * z + 1 - c, t)
    tx, ty, td = flipped(t, 1), flipped(t, 2), flipped(t, 3)
    always = z >= 0

    def other_stack(k):
        return lax.rem(z + k, stacks)

    others = [(partner, always)] + [((sp, u), always) for u in (tx, ty, td)]
    for k in range(1, stacks):
        for core in (c, 1 - c):
            others.append(((2 * other_stack(k) + core, t), always))
    greet(others)

    def remote(src, dst, send, recv, device):
        return pltpu.make_async_remote_copy(
            src_ref=src, dst_ref=dst, send_sem=send, recv_sem=recv,
            device_id=device, device_id_type=MESH,
        )

    def span(d, core):
        return pl.ds(pl.multiple_of((2 * d + core) * rows, 16), rows)

    def wide(q):
        return pl.ds(pl.multiple_of(q * quarter, 128), quarter)

    def part(q, p):
        return pl.ds(pl.multiple_of(q * quarter + p * half, 128), half)

    order = list(range(1, stacks)) + [0]

    def swap(k):
        return remote(p_ref.at[span(other_stack(k), 1 - c), :], theirs.at[k], ps.at[k], pr.at[k], partner)

    def read(k):
        return pltpu.make_async_copy(p_ref.at[span(other_stack(k), c), :], ours.at[k], load.at[k])

    def via_x(k):
        return remote(out_b.at[k], in_x.at[k], bs.at[k], br.at[k], (sp, tx))

    def via_y(k):
        return remote(out_a.at[k], in_y.at[k], as_.at[k], ar.at[k], (sp, ty))

    def to_x(k):
        return remote(summed.at[k, 0], got_x.at[k], xs.at[k], xr.at[k], (sp, tx))

    def to_y(k):
        return remote(summed.at[k, 1], got_y.at[k], ys.at[k], yr.at[k], (sp, ty))

    def home(k):
        back = stacks - k
        return remote(block.at[k], blocks.at[k], zs.at[k], zr.at[k], (2 * other_stack(k) + c, t))

    def both(k, at):
        return ours[k, :, at].astype(jnp.float32) + theirs[k, :, at].astype(jnp.float32)

    def stage_one(k):
        read(k).wait()
        swap(k).wait_recv()
        out_a[k] = both(k, part(td, 0)).astype(jnp.bfloat16)
        via_y(k).start()
        out_b[k] = both(k, part(td, 1)).astype(jnp.bfloat16)
        via_x(k).start()

    def stage_two(k):
        summed[k, 0, :, half:] = both(k, part(tx, 1)).astype(jnp.bfloat16)
        summed[k, 1, :, :half] = both(k, part(ty, 0)).astype(jnp.bfloat16)
        via_y(k).wait_recv()
        summed[k, 0, :, :half] = (both(k, part(tx, 0)) + in_y[k].astype(jnp.float32)).astype(jnp.bfloat16)
        to_x(k).start()
        via_x(k).wait_recv()
        summed[k, 1, :, half:] = (both(k, part(ty, 1)) + in_x[k].astype(jnp.float32)).astype(jnp.bfloat16)
        to_y(k).start()

    def stage_three(k):
        mine = both(k, wide(t))
        to_x(k).wait_recv()
        to_y(k).wait_recv()
        mine = mine + got_x[k].astype(jnp.float32) + got_y[k].astype(jnp.float32)
        block[k] = mine.astype(jnp.bfloat16)
        if k:
            home(k).start()

    for k in order:
        swap(k).start()
        read(k).start()
    for i in range(stacks + 2):
        for stage, lag in ((stage_one, 0), (stage_two, 1), (stage_three, 2)):
            if 0 <= i - lag < stacks:
                stage(order[i - lag])
    total = c_ref[:, wide(t)].astype(jnp.float32) + block[0].astype(jnp.float32)
    for k in range(1, stacks):
        home(k).wait_recv()
        total = total + blocks[k].astype(jnp.float32)
    cols[...] = total.astype(jnp.bfloat16)

    gathers = []
    for i, u in enumerate((td, tx, ty)):
        gathers.append(remote(cols, stream.at[:, wide(t)], gs.at[i], gr.at[i], (sp, u)))
        gathers[-1].start()
    keep = pltpu.make_async_copy(cols, stream.at[:, wide(t)], local.at[0])
    keep.start()
    for copy in gathers:
        copy.wait()
    keep.wait()
    share = columns.shape[1]

    def slab(device):
        return stream.at[:, pl.ds(pl.multiple_of(device * share, 128), share)]

    mine = columns.at[pl.ds(pl.multiple_of(sp * rows, 16), rows), :]
    sends = []
    n = 0
    for k in (2, 1, 3, 0) if stacks == 4 else range(stacks):
        for core in (c, 1 - c) if k else (1 - c,):
            device = 2 * other_stack(k) + core
            sends.append(remote(slab(device), mine, es.at[n], er.at[n], (device, t)))
            sends[-1].start()
            n += 1
    keep = pltpu.make_async_copy(slab(sp), mine, local.at[1])
    keep.start()
    for k in order:
        swap(k).wait_send()
        via_x(k).wait_send()
        via_y(k).wait_send()
        to_x(k).wait_send()
        to_y(k).wait_send()
        if k:
            home(k).wait_send()
    for copy in sends:
        copy.wait()
    keep.wait()


def dense_plan(
    moe_input, cotangent, route_ids, route_weights, expert_gate, expert_up,
    expert_down, out_proj, gate_b, gate_c, conv_in, taps,
):
    groups = lax.axis_size("sp")
    stacks = groups // 2
    rows, width = moe_input.shape
    quarter = width // lax.axis_size("tp")
    tokens = rows * groups
    bf16 = jnp.bfloat16
    any_space = pl.BlockSpec(memory_space=pl.ANY)
    vmem = pl.BlockSpec(memory_space=pltpu.VMEM)
    dma = pltpu.SemaphoreType.DMA

    mixed = gate_c.astype(jnp.float32) * conv_in.astype(jnp.float32)
    earlier_rows = passed_along(mixed[-2:], "sp", 1)
    extended = jnp.concatenate([earlier_rows, mixed], axis=0)
    conv = taps[2] * mixed + taps[1] * extended[1:-1] + taps[0] * extended[:-2]
    merged = (gate_b.astype(jnp.float32) * conv).astype(bf16)

    ids = lax.all_gather(route_ids, "sp", axis=0, tiled=True)
    weights = lax.all_gather(route_weights, "sp", axis=0, tiled=True)
    chosen = jnp.sum(jnp.where(ids == lax.axis_index("sp"), weights, 0.0), axis=1, keepdims=True)

    n = 6 * (stacks - 1)
    rows_x, all_cot, all_merged = pl.pallas_call(
        functools.partial(gather_kernel, stacks),
        out_shape=(
            jax.ShapeDtypeStruct((tokens, width), bf16),
            jax.ShapeDtypeStruct((tokens, width), bf16),
            jax.ShapeDtypeStruct((tokens, quarter), bf16),
        ),
        in_specs=[vmem] * 3,
        out_specs=(any_space,) * 3,
        scratch_shapes=[dma((n,))] * 10 + [dma((4 * n,))] * 2 + [dma((3,))] * 3,
        compiler_params=pltpu.CompilerParams(collective_id=0, has_side_effects=True),
    )(moe_input, cotangent, merged)

    rows_s = (chosen * all_cot.astype(jnp.float32)).astype(bf16)
    weight_gate, weight_up, weight_down = expert_gate[0], expert_up[0], expert_down[0]
    pre_gate = jnp.dot(rows_x, weight_gate, preferred_element_type=jnp.float32)
    pre_up = jnp.dot(rows_x, weight_up, preferred_element_type=jnp.float32)
    sigma = jax.nn.sigmoid(pre_gate)
    active = pre_gate * sigma
    hidden = (active * pre_up).astype(bf16)
    back = contract(rows_s, weight_down, 1, 1)
    grad_pre_gate = (back * pre_up * sigma * (1.0 + pre_gate * (1.0 - sigma))).astype(bf16)
    grad_pre_up = (back * active).astype(bf16)
    partial_value = (
        contract(grad_pre_gate, weight_gate, 1, 1) + contract(grad_pre_up, weight_up, 1, 1)
    ).astype(bf16)
    grad_down = contract(hidden, rows_s, 0, 0)
    grad_gate = contract(rows_x, grad_pre_gate, 0, 0)
    grad_up = contract(rows_x, grad_pre_up, 0, 0)

    half = quarter // 2
    share = width // groups
    scratch = [
        pltpu.VMEM((stacks, rows, width), bf16),
        pltpu.VMEM((stacks, rows, width), bf16),
        pltpu.VMEM((stacks, 2, rows, quarter), bf16),
    ]
    scratch += [pltpu.VMEM((stacks, rows, half), bf16)] * 4
    scratch += [pltpu.VMEM((stacks, rows, quarter), bf16)] * 4
    scratch += [pltpu.VMEM((rows, quarter), bf16)]
    scratch += [dma((stacks,))] * 12 + [dma((3,))] * 2 + [dma((groups - 1,))] * 2
    scratch += [dma((2,)), dma((stacks,))]
    stream_grad, stream_cols = pl.pallas_call(
        functools.partial(return_kernel, stacks),
        out_shape=(
            jax.ShapeDtypeStruct((rows, width), bf16),
            jax.ShapeDtypeStruct((tokens, share), bf16),
        ),
        in_specs=[any_space, vmem],
        out_specs=(any_space, any_space),
        scratch_shapes=scratch,
        compiler_params=pltpu.CompilerParams(collective_id=1, has_side_effects=True),
    )(partial_value, cotangent)

    grad_merged = contract(stream_grad, out_proj, 1, 1)
    grad_gate_b = (grad_merged * conv).astype(bf16)
    grad_conv = grad_merged * gate_b.astype(jnp.float32)
    later_rows = passed_along(grad_conv[:2], "sp", -1)
    extended_grad = jnp.concatenate([grad_conv, later_rows], axis=0)
    grad_mixed = taps[2] * grad_conv + taps[1] * extended_grad[1:-1] + taps[0] * extended_grad[2:]
    grad_gate_c = (grad_mixed * conv_in.astype(jnp.float32)).astype(bf16)
    grad_conv_in = (grad_mixed * gate_c.astype(jnp.float32)).astype(bf16)
    grad_proj = contract(all_merged, stream_cols, 0, 0)
    return (
        grad_gate[None], grad_up[None], grad_down[None], grad_proj,
        grad_gate_b, grad_gate_c, grad_conv_in,
    )


def on_device(*args):
    rows, choices = args[2].shape
    groups, lanes = lax.axis_size("sp"), lax.axis_size("tp")
    slots = 2 * rows * choices
    if lanes == 4 and groups % 2 == 0 and groups > 2 and rows * groups <= 2 * slots:
        return dense_plan(*args)
    return slot_plan(*args)


def solution(mesh):
    placed = (
        P("sp", None),
        P("sp", None),
        P("sp", None),
        P("sp", None),
        P("sp", None, "tp"),
        P("sp", None, "tp"),
        P("sp", "tp", None),
        P("tp", None),
        P("sp", "tp"),
        P("sp", "tp"),
        P("sp", "tp"),
        P(None, "tp"),
    )
    return jax.shard_map(
        on_device,
        mesh=mesh,
        in_specs=placed,
        out_specs=(
            P("sp", None, "tp"),
            P("sp", None, "tp"),
            P("sp", "tp", None),
            P("tp", "sp"),
            P("sp", "tp"),
            P("sp", "tp"),
            P("sp", "tp"),
        ),
        check_vma=False,
    )
```

```python
import functools
import jax
import jax.numpy as jnp
from jax import lax
from jax.experimental import pallas as pl
from jax.experimental.pallas import tpu as pltpu
from jax.sharding import PartitionSpec as P

EXP_DEV = 1


def passed_along(block, axis, distance):
    devices = range(lax.axis_size(axis))
    route = [(i - distance, i) for i in devices if i - distance in devices]
    return lax.ppermute(block, axis, route)


def slot_table(routes, experts, capacity):
    flattened = routes.reshape(-1)
    onehot = (flattened[:, None] == jnp.arange(experts, dtype=jnp.int32)[None, :]).astype(jnp.int32)
    earlier = jnp.cumsum(onehot, axis=0) - onehot
    return flattened * capacity + jnp.sum(earlier * onehot, axis=1)


def contract(left, right, left_dim, right_dim):
    return lax.dot_general(
        left, right, (((left_dim,), (right_dim,)), ((), ())), preferred_element_type=jnp.float32
    )


def slot_plan(
    moe_input,
    cotangent,
    route_ids,
    route_weights,
    expert_gate,
    expert_up,
    expert_down,
    out_proj,
    gate_b,
    gate_c,
    conv_in,
    taps,
):
    groups = lax.axis_size("sp")
    lanes = lax.axis_size("tp")
    token_count, model_width = moe_input.shape
    choices_count = route_ids.shape[1]
    experts = EXP_DEV * groups
    capacity = 2 * token_count * choices_count // experts
    assigned = token_count * choices_count
    slice_width = model_width // lanes
    column_start = lax.axis_index("tp") * slice_width
    slots = slot_table(route_ids, experts, capacity)
    owner = (
        jnp.full((experts * capacity,), assigned, jnp.int32)
        .at[slots]
        .set(jnp.arange(assigned, dtype=jnp.int32))
    )
    token_owner = jnp.where(owner < assigned, owner // choices_count, token_count)
    scaled = (
        (route_weights[:, :, None] * cotangent[:, None, :].astype(jnp.float32))
        .astype(jnp.bfloat16)
        .reshape(assigned, model_width)
    )

    def to_slots(values, positions):
        padded = jnp.concatenate([values, jnp.zeros((1, values.shape[1]), values.dtype)], axis=0)
        return padded[positions].reshape(experts, capacity, values.shape[1])

    slim_x = to_slots(
        lax.dynamic_slice_in_dim(moe_input, column_start, slice_width, 1), token_owner
    )
    slim_s = to_slots(lax.dynamic_slice_in_dim(scaled, column_start, slice_width, 1), owner)
    part_x, part_s = (
        lax.all_to_all(slim_x, "sp", split_axis=0, concat_axis=0, tiled=True),
        lax.all_to_all(slim_s, "sp", split_axis=0, concat_axis=0, tiled=True),
    )
    arrived_x, arrived_s = (
        lax.all_gather(part_x, "tp", axis=2, tiled=True),
        lax.all_gather(part_s, "tp", axis=2, tiled=True),
    )
    rows_x = arrived_x.reshape(-1, model_width)
    rows_s = arrived_s.reshape(-1, model_width)
    weight_gate = expert_gate[0]
    weight_up = expert_up[0]
    weight_down = expert_down[0]
    pre_gate = jnp.dot(rows_x, weight_gate, preferred_element_type=jnp.float32)
    pre_up = jnp.dot(rows_x, weight_up, preferred_element_type=jnp.float32)
    sigma = jax.nn.sigmoid(pre_gate)
    active = pre_gate * sigma
    hidden = (active * pre_up).astype(jnp.bfloat16)
    back = contract(rows_s, weight_down, 1, 1)
    grad_pre_gate = (back * pre_up * sigma * (1.0 + pre_gate * (1.0 - sigma))).astype(jnp.bfloat16)
    grad_pre_up = (back * active).astype(jnp.bfloat16)
    grad_down = contract(hidden, rows_s, 0, 0)
    grad_gate = contract(rows_x, grad_pre_gate, 0, 0)
    grad_up = contract(rows_x, grad_pre_up, 0, 0)
    partial_value = contract(grad_pre_gate, weight_gate, 1, 1) + contract(
        grad_pre_up, weight_up, 1, 1
    )
    summed = lax.psum_scatter(
        partial_value.astype(jnp.bfloat16), "tp", scatter_dimension=1, tiled=True
    )
    returned = lax.all_to_all(
        summed.reshape(groups, capacity, slice_width), "sp", split_axis=0, concat_axis=0, tiled=True
    )
    returned = returned.reshape(experts * capacity, slice_width)
    moe_rows = (
        returned[slots]
        .astype(jnp.float32)
        .reshape(token_count, choices_count, slice_width)
        .sum(axis=1)
    )
    own_cols = lax.dynamic_slice_in_dim(cotangent, column_start, slice_width, 1)
    grad_cols = (own_cols.astype(jnp.float32) + moe_rows).astype(jnp.bfloat16)
    stream_grad = lax.all_gather(grad_cols, "tp", axis=1, tiled=True)
    mixed = gate_c.astype(jnp.float32) * conv_in.astype(jnp.float32)
    earlier_rows = passed_along(mixed[-2:], "sp", 1)
    extended = jnp.concatenate([earlier_rows, mixed], axis=0)
    conv = taps[2] * mixed + taps[1] * extended[1:-1] + taps[0] * extended[:-2]
    merged = (gate_b.astype(jnp.float32) * conv).astype(jnp.bfloat16)
    grad_merged = contract(stream_grad, out_proj, 1, 1)
    grad_gate_b = (grad_merged * conv).astype(jnp.bfloat16)
    grad_conv = grad_merged * gate_b.astype(jnp.float32)
    later_rows = passed_along(grad_conv[:2], "sp", -1)
    extended_grad = jnp.concatenate([grad_conv, later_rows], axis=0)
    grad_mixed = taps[2] * grad_conv + taps[1] * extended_grad[1:-1] + taps[0] * extended_grad[2:]
    grad_gate_c = (grad_mixed * conv_in.astype(jnp.float32)).astype(jnp.bfloat16)
    grad_conv_in = (grad_mixed * gate_c.astype(jnp.float32)).astype(jnp.bfloat16)
    grad_proj = lax.psum_scatter(
        contract(stream_grad, merged, 0, 0).astype(jnp.bfloat16),
        "sp",
        scatter_dimension=0,
        tiled=True,
    ).astype(jnp.float32)
    return (
        grad_gate[None],
        grad_up[None],
        grad_down[None],
        grad_proj.T,
        grad_gate_b,
        grad_gate_c,
        grad_conv_in,
    )


MESH = pl.DeviceIdType.MESH


def place():
    sp, t = lax.axis_index("sp"), lax.axis_index("tp")
    return sp, lax.div(sp, 2), lax.rem(sp, 2), t


def flipped(t, bits):
    x, y = lax.rem(t, 2), lax.div(t, 2)
    if bits & 1:
        x = 1 - x
    if bits & 2:
        y = 1 - y
    return 2 * y + x


def greet(devices):
    barrier = pltpu.get_barrier_semaphore()
    for device, exists in devices:
        @pl.when(exists)
        def _():
            pl.semaphore_signal(barrier, inc=1, device_id=device, device_id_type=MESH)
    pl.semaphore_wait(barrier, sum([jnp.where(exists, 1, 0) for _, exists in devices]))


def gather_kernel(
    stacks, x_ref, s_ref, w_ref, full_x, full_s, full_w,
    zs, zr, xs, xr, ys, yr, ax, ar, bx, br, cs, cr, ws, wr, own_s, own_r, local,
):
    sp, z, c, t = place()
    rows, width = x_ref.shape
    quarter = width // 4
    half = quarter // 2
    partner = (2 * z + 1 - c, t)
    up, down = (sp + 2, t), (sp - 2, t)
    tx, ty, td = flipped(t, 1), flipped(t, 2), flipped(t, 3)
    always = z >= 0
    peers = [(lax.rem(sp + k, 2 * stacks), t) for k in range(1, 2 * stacks)]
    greet([(peer, always) for peer in peers + [(sp, tx), (sp, ty)]])
    ins, outs = (x_ref, s_ref), (full_x, full_s)

    def cols(q, part=None):
        if part is None:
            return pl.ds(pl.multiple_of(q * quarter, 128), quarter)
        return pl.ds(pl.multiple_of(q * quarter + part * half, 128), half)

    def span(d):
        return pl.ds(pl.multiple_of((2 * d + c) * rows, 16), rows)

    def remote(src, dst, send, recv, device):
        return pltpu.make_async_remote_copy(
            src_ref=src, dst_ref=dst, send_sem=send, recv_sem=recv,
            device_id=device, device_id_type=MESH,
        )

    def region(a, d, q, part=None):
        return outs[a].at[span(d), cols(q, part)]

    def mine(a):
        return ins[a].at[:, cols(t)]

    def slot(a, way, k):
        return (a * 2 + way) * (stacks - 1) + k

    def zcopy(a, way, k, src, d):
        i = slot(a, way, k)
        return remote(src, region(a, d, t), zs.at[i], zr.at[i], up if way == 0 else down)

    def ahead(way):
        return z < stacks - 1 if way == 0 else z > 0

    def source(way, k):
        return z - 1 - k if way == 0 else z + 1 + k

    def exists(way, k):
        return z >= k + 1 if way == 0 else z + 1 + k < stacks

    order = (0, 1)
    for a in order:
        for way in (0, 1):
            @pl.when(ahead(way))
            def _():
                zcopy(a, way, 0, mine(a), z).start()
    keeps = []
    for k, peer in enumerate(peers):
        keeps.append(remote(w_ref, full_w.at[sp], ws.at[k], wr.at[k], peer))
        keeps[-1].start()
    keeps.append(pltpu.make_async_copy(w_ref, full_w.at[sp], local.at[2]))
    keeps[-1].start()
    for a in order:
        dst = outs[a].at[span(z), :]
        keeps.append(pltpu.make_async_copy(ins[a], dst, local.at[a]))
        keeps[-1].start()
        keeps.append(remote(ins[a], dst, own_s.at[a], own_r.at[a], partner))
        keeps[-1].start()

    def xy(a, way, k, d, kind):
        i = slot(a, way, k)
        if kind == "x":
            r = region(a, d, t)
            return remote(r, r, xs.at[i], xr.at[i], (sp, tx))
        if kind == "y":
            r = region(a, d, t)
            return remote(r, r, ys.at[i], yr.at[i], (sp, ty))
        if kind == "a":
            r = region(a, d, tx, 0)
            return remote(r, r, ax.at[i], ar.at[i], (sp, ty))
        r = region(a, d, ty, 1)
        return remote(r, r, bx.at[i], br.at[i], (sp, tx))

    def shared(a, way, k, d, which):
        i = 4 * slot(a, way, k) + which
        r = region(a, d, (t, tx, ty, td)[which])
        return remote(r, r, cs.at[i], cr.at[i], partner)

    def first(a, way, k):
        d = source(way, k)
        zcopy(a, way, k, region(a, d, t), d).wait_recv()
        if k < stacks - 2:
            @pl.when(ahead(way))
            def _():
                zcopy(a, way, k + 1, region(a, d, t), d).start()
        xy(a, way, k, d, "x").start()
        xy(a, way, k, d, "y").start()
        shared(a, way, k, d, 0).start()

    def second(a, way, k):
        d = source(way, k)
        xy(a, way, k, d, "x").wait_recv()
        xy(a, way, k, d, "a").start()
        shared(a, way, k, d, 1).start()
        xy(a, way, k, d, "y").wait_recv()
        xy(a, way, k, d, "b").start()
        shared(a, way, k, d, 2).start()

    def third(a, way, k):
        d = source(way, k)
        xy(a, way, k, d, "a").wait_recv()
        xy(a, way, k, d, "b").wait_recv()
        shared(a, way, k, d, 3).start()

    steps = [(a, way, k) for k in range(stacks - 1) for a in order for way in (0, 1)]
    for i in range(len(steps) + 4):
        for stage, lag in ((first, 0), (second, 2), (third, 4)):
            if 0 <= i - lag < len(steps):
                a, way, k = steps[i - lag]
                @pl.when(exists(way, k))
                def _():
                    stage(a, way, k)
    for copy in keeps:
        copy.wait()
    for a, way, k in steps:
        passed = z >= k if way == 0 else z + k < stacks

        @pl.when(passed & ahead(way))
        def _():
            d = z - k if way == 0 else z + k
            zcopy(a, way, k, region(a, d, t), d).wait_send()

        @pl.when(exists(way, k))
        def _():
            d = source(way, k)
            for kind in "xyab":
                xy(a, way, k, d, kind).wait_send()
            for which in range(4):
                shared(a, way, k, d, which).wait()


def return_kernel(
    stacks, p_ref, c_ref, m_ref, w_ref, conv_ref, gb_ref, gc_ref, ci_ref, taps_ref,
    columns, full_m, dgb_ref, dgc_ref, dci_ref,
    theirs, ours, summed, in_x, in_y, out_a, out_b, got_x, got_y, block, blocks, stream, ext,
    ps, pr, as_, ar, bs, br, xs, xr, ys, yr, zs, zr, ms, mr, ns, nr, gs, gr, es, er, local, load, hs, hr,
):
    sp, z, c, t = place()
    rows, width = p_ref.shape[0] // (2 * stacks), p_ref.shape[1]
    quarter = width // 4
    half = quarter // 2
    partner = (2 * z + 1 - c, t)
    tx, ty, td = flipped(t, 1), flipped(t, 2), flipped(t, 3)
    always = z >= 0

    def other_stack(k):
        return lax.rem(z + k, stacks)

    others = [(partner, always)] + [((sp, u), always) for u in (tx, ty, td)]
    for k in range(1, stacks):
        for core in (c, 1 - c):
            others.append(((2 * other_stack(k) + core, t), always))
    greet(others)

    def remote(src, dst, send, recv, device):
        return pltpu.make_async_remote_copy(
            src_ref=src, dst_ref=dst, send_sem=send, recv_sem=recv,
            device_id=device, device_id_type=MESH,
        )

    def span(d, core):
        return pl.ds(pl.multiple_of((2 * d + core) * rows, 16), rows)

    def wide(q):
        return pl.ds(pl.multiple_of(q * quarter, 128), quarter)

    def part(q, p):
        return pl.ds(pl.multiple_of(q * quarter + p * half, 128), half)

    order = list(range(1, stacks)) + [0]

    def swap(k):
        return remote(p_ref.at[span(other_stack(k), 1 - c), :], theirs.at[k], ps.at[k], pr.at[k], partner)

    def read(k):
        return pltpu.make_async_copy(p_ref.at[span(other_stack(k), c), :], ours.at[k], load.at[k])

    def via_x(k):
        return remote(out_b.at[k], in_x.at[k], bs.at[k], br.at[k], (sp, tx))

    def via_y(k):
        return remote(out_a.at[k], in_y.at[k], as_.at[k], ar.at[k], (sp, ty))

    def to_x(k):
        return remote(summed.at[k, 0], got_x.at[k], xs.at[k], xr.at[k], (sp, tx))

    def to_y(k):
        return remote(summed.at[k, 1], got_y.at[k], ys.at[k], yr.at[k], (sp, ty))

    def home(k):
        back = stacks - k
        return remote(block.at[k], blocks.at[k], zs.at[k], zr.at[k], (2 * other_stack(k) + c, t))

    def both(k, at):
        return ours[k, :, at].astype(jnp.float32) + theirs[k, :, at].astype(jnp.float32)

    def stage_one(k):
        read(k).wait()
        swap(k).wait_recv()
        out_a[k] = both(k, part(td, 0)).astype(jnp.bfloat16)
        via_y(k).start()
        out_b[k] = both(k, part(td, 1)).astype(jnp.bfloat16)
        via_x(k).start()

    def stage_two(k):
        summed[k, 0, :, half:] = both(k, part(tx, 1)).astype(jnp.bfloat16)
        summed[k, 1, :, :half] = both(k, part(ty, 0)).astype(jnp.bfloat16)
        via_y(k).wait_recv()
        summed[k, 0, :, :half] = (both(k, part(tx, 0)) + in_y[k].astype(jnp.float32)).astype(jnp.bfloat16)
        to_x(k).start()
        via_x(k).wait_recv()
        summed[k, 1, :, half:] = (both(k, part(ty, 1)) + in_x[k].astype(jnp.float32)).astype(jnp.bfloat16)
        to_y(k).start()

    def stage_three(k):
        mine = both(k, wide(t))
        to_x(k).wait_recv()
        to_y(k).wait_recv()
        mine = mine + got_x[k].astype(jnp.float32) + got_y[k].astype(jnp.float32)
        block[k] = mine.astype(jnp.bfloat16)
        if k:
            home(k).start()

    for k in order:
        swap(k).start()
        read(k).start()

    def behind(k):
        return lax.rem(z + stacks - k, stacks)

    def merged_out(k):
        return remote(m_ref, full_m.at[span(z, c), :], ms.at[k], mr.at[k], (2 * other_stack(k) + c, t))

    def merged_on(k):
        r = full_m.at[span(behind(k), c), :]
        return remote(r if k else m_ref, r, ns.at[k], nr.at[k], partner)

    for k in range(1, stacks):
        merged_out(k).start()
    merged_on(0).start()
    keep_m = pltpu.make_async_copy(m_ref, full_m.at[span(z, c), :], local.at[0])
    keep_m.start()
    for i in range(stacks + 2):
        for stage, lag in ((stage_one, 0), (stage_two, 1), (stage_three, 2)):
            if 0 <= i - lag < stacks:
                stage(order[i - lag])
    total = c_ref[:, wide(t)].astype(jnp.float32) + block[0].astype(jnp.float32)
    for k in range(1, stacks):
        home(k).wait_recv()
        total = total + blocks[k].astype(jnp.float32)
    stream[:, wide(t)] = total.astype(jnp.bfloat16)

    gathers = []
    for i, u in enumerate((td, tx, ty)):
        own = stream.at[:, wide(t)]
        gathers.append(remote(own, own, gs.at[i], gr.at[i], (sp, u)))
        gathers[-1].start()
    for k in range(1, stacks):
        merged_out(k).wait_recv()
        merged_on(k).start()
    for copy in gathers:
        copy.wait()
    share = columns.shape[1]

    def slab(device):
        return stream.at[:, pl.ds(pl.multiple_of(device * share, 128), share)]

    mine = columns.at[pl.ds(pl.multiple_of(sp * rows, 16), rows), :]
    sends = []
    n = 0
    for k in (2, 1, 3, 0) if stacks == 4 else range(stacks):
        for core in (c, 1 - c) if k else (1 - c,):
            device = 2 * other_stack(k) + core
            sends.append(remote(slab(device), mine, es.at[n], er.at[n], (device, t)))
            sends[-1].start()
            n += 1
    keep = pltpu.make_async_copy(slab(sp), mine, local.at[1])
    keep.start()

    last = 2 * stacks - 1
    halo = remote(
        ext.at[pl.ds(0, 8), :], ext.at[pl.ds(rows, 8), :], hs.at[0], hr.at[0], (jnp.maximum(sp - 1, 0), t)
    )
    grad_merged = contract(stream[...], w_ref[...], 1, 1)
    ext[pl.ds(0, rows), :] = grad_merged * gb_ref[...].astype(jnp.float32)

    @pl.when(sp > 0)
    def _():
        halo.start()

    dgb_ref[...] = (grad_merged * conv_ref[...]).astype(jnp.bfloat16)

    @pl.when(sp == last)
    def _():
        ext[pl.ds(rows, 8), :] = jnp.zeros((8, quarter), jnp.float32)

    @pl.when(sp < last)
    def _():
        halo.wait_recv()

    grad_mixed = (
        taps_ref[2:3, :] * ext[pl.ds(0, rows), :]
        + taps_ref[1:2, :] * ext[pl.ds(1, rows), :]
        + taps_ref[0:1, :] * ext[pl.ds(2, rows), :]
    )
    dgc_ref[...] = (grad_mixed * ci_ref[...].astype(jnp.float32)).astype(jnp.bfloat16)
    dci_ref[...] = (grad_mixed * gc_ref[...].astype(jnp.float32)).astype(jnp.bfloat16)

    @pl.when(sp > 0)
    def _():
        halo.wait_send()

    keep_m.wait()
    for k in range(stacks):
        if k:
            merged_out(k).wait_send()
        merged_on(k).wait()
    for k in order:
        swap(k).wait_send()
        via_x(k).wait_send()
        via_y(k).wait_send()
        to_x(k).wait_send()
        to_y(k).wait_send()
        if k:
            home(k).wait_send()
    for copy in sends:
        copy.wait()
    keep.wait()


def dense_plan(
    moe_input, cotangent, route_ids, route_weights, expert_gate, expert_up,
    expert_down, out_proj, gate_b, gate_c, conv_in, taps,
):
    groups = lax.axis_size("sp")
    stacks = groups // 2
    rows, width = moe_input.shape
    quarter = width // lax.axis_size("tp")
    tokens = rows * groups
    bf16 = jnp.bfloat16
    any_space = pl.BlockSpec(memory_space=pl.ANY)
    vmem = pl.BlockSpec(memory_space=pltpu.VMEM)
    dma = pltpu.SemaphoreType.DMA

    mixed = gate_c.astype(jnp.float32) * conv_in.astype(jnp.float32)
    earlier_rows = passed_along(mixed[-2:], "sp", 1)
    extended = jnp.concatenate([earlier_rows, mixed], axis=0)
    conv = taps[2] * mixed + taps[1] * extended[1:-1] + taps[0] * extended[:-2]
    merged = (gate_b.astype(jnp.float32) * conv).astype(bf16)

    named = jnp.arange(groups, dtype=jnp.int32)[:, None, None] == route_ids.T[None]
    table = jnp.sum(jnp.where(named, route_weights.T[None], 0.0), axis=1)

    n = 4 * (stacks - 1)
    rows_x, rows_c, tables = pl.pallas_call(
        functools.partial(gather_kernel, stacks),
        out_shape=(
            jax.ShapeDtypeStruct((tokens, width), bf16),
            jax.ShapeDtypeStruct((tokens, width), bf16),
            jax.ShapeDtypeStruct((groups, groups, rows), jnp.float32),
        ),
        in_specs=[vmem] * 3,
        out_specs=(any_space, any_space, vmem),
        scratch_shapes=[dma((n,))] * 10 + [dma((4 * n,))] * 2 + [dma((groups - 1,))] * 2 + [dma((3,))] * 3,
        compiler_params=pltpu.CompilerParams(collective_id=0, has_side_effects=True),
    )(moe_input, cotangent, table)
    chosen = lax.dynamic_index_in_dim(tables, lax.axis_index("sp"), 1, keepdims=False)
    chosen = chosen.reshape(tokens, 1)

    weight_gate, weight_up, weight_down = expert_gate[0], expert_up[0], expert_down[0]
    pre_gate = jnp.dot(rows_x, weight_gate, preferred_element_type=jnp.float32)
    pre_up = jnp.dot(rows_x, weight_up, preferred_element_type=jnp.float32)
    sigma = jax.nn.sigmoid(pre_gate)
    active = pre_gate * sigma
    hidden = (chosen * (active * pre_up)).astype(bf16)
    back = chosen * contract(rows_c, weight_down, 1, 1)
    grad_pre_gate = (back * pre_up * sigma * (1.0 + pre_gate * (1.0 - sigma))).astype(bf16)
    grad_pre_up = (back * active).astype(bf16)
    partial_value = (
        contract(grad_pre_gate, weight_gate, 1, 1) + contract(grad_pre_up, weight_up, 1, 1)
    ).astype(bf16)
    grad_down = contract(hidden, rows_c, 0, 0)
    grad_gate = contract(rows_x, grad_pre_gate, 0, 0)
    grad_up = contract(rows_x, grad_pre_up, 0, 0)

    half = quarter // 2
    share = width // groups
    scratch = [
        pltpu.VMEM((stacks, rows, width), bf16),
        pltpu.VMEM((stacks, rows, width), bf16),
        pltpu.VMEM((stacks, 2, rows, quarter), bf16),
    ]
    scratch += [pltpu.VMEM((stacks, rows, half), bf16)] * 4
    scratch += [pltpu.VMEM((stacks, rows, quarter), bf16)] * 4
    scratch += [pltpu.VMEM((rows, width), bf16), pltpu.VMEM((rows + 8, quarter), jnp.float32)]
    scratch += [dma((stacks,))] * 16 + [dma((3,))] * 2 + [dma((groups - 1,))] * 2
    scratch += [dma((2,)), dma((stacks,)), dma((1,)), dma((1,))]
    token_block = jax.ShapeDtypeStruct((rows, quarter), bf16)
    stream_cols, all_merged, grad_gate_b, grad_gate_c, grad_conv_in = pl.pallas_call(
        functools.partial(return_kernel, stacks),
        out_shape=(
            jax.ShapeDtypeStruct((tokens, share), bf16),
            jax.ShapeDtypeStruct((tokens, quarter), bf16),
            token_block, token_block, token_block,
        ),
        in_specs=[any_space] + [vmem] * 8,
        out_specs=(any_space, any_space, vmem, vmem, vmem),
        scratch_shapes=scratch,
        compiler_params=pltpu.CompilerParams(collective_id=1, has_side_effects=True),
    )(partial_value, cotangent, merged, out_proj, conv, gate_b, gate_c, conv_in, taps)

    grad_proj = contract(all_merged, stream_cols, 0, 0)
    return (
        grad_gate[None], grad_up[None], grad_down[None], grad_proj,
        grad_gate_b, grad_gate_c, grad_conv_in,
    )


def on_device(*args):
    rows, choices = args[2].shape
    groups, lanes = lax.axis_size("sp"), lax.axis_size("tp")
    slots = 2 * rows * choices
    if lanes == 4 and groups % 2 == 0 and groups > 2 and rows * groups <= 2 * slots:
        return dense_plan(*args)
    return slot_plan(*args)


def solution(mesh):
    placed = (
        P("sp", None),
        P("sp", None),
        P("sp", None),
        P("sp", None),
        P("sp", None, "tp"),
        P("sp", None, "tp"),
        P("sp", "tp", None),
        P("tp", None),
        P("sp", "tp"),
        P("sp", "tp"),
        P("sp", "tp"),
        P(None, "tp"),
    )
    return jax.shard_map(
        on_device,
        mesh=mesh,
        in_specs=placed,
        out_specs=(
            P("sp", None, "tp"),
            P("sp", None, "tp"),
            P("sp", "tp", None),
            P("tp", "sp"),
            P("sp", "tp"),
            P("sp", "tp"),
            P("sp", "tp"),
        ),
        check_vma=False,
    )
```
